32 devices in a mesh: rep: 2 (over x), fs: 8 (over z, y), tp: 2 (over core).
Axes of the slice: x: 2, y: 2, z: 4, core: 2. Of those that a mesh axis runs over, the one named last changes fastest.
Arguments:
- pre_gate: bfloat16 [12288, 4096], P(('rep', 'fs'), 'tp'), may hold values from -6 to 6
- pre_linear: bfloat16 [12288, 4096], P(('rep', 'fs'), 'tp'), may hold values from -6 to 6
- taps_gate: float32 [3, 4096], P(None, 'tp'), may hold values from -3.5 to 3.5
- taps_linear: float32 [3, 4096], P(None, 'tp'), may hold values from -3.5 to 3.5
- bias_gate: float32 [4096], P('tp'), may hold values from -3 to 3
- bias_linear: float32 [4096], P('tp'), may hold values from -3 to 3
- down_weight: bfloat16 [4096, 2048], P('tp', 'fs'), may hold values from -0.09375 to 0.09375
- out_grad: bfloat16 [12288, 2048], P(('rep', 'fs')), may hold values from -8 to 8
Outputs:
- grad_gate: bfloat16 [12288, 4096], P(('rep', 'fs'), 'tp')
- grad_linear: bfloat16 [12288, 4096], P(('rep', 'fs'), 'tp')
- grad_taps_gate: float32 [3, 4096], P(None, 'tp')
- grad_taps_linear: float32 [3, 4096], P(None, 'tp')
- grad_bias_gate: float32 [4096], P('tp')
- grad_bias_linear: float32 [4096], P('tp')
- grad_down: float32 [4096, 2048], P('tp', 'fs')
- row_norms: float32 [4096], P('tp')
The draws below stay inside these ranges and needn't reach their ends.
All inputs are finite; a program needn't handle non-finite values.
Results may differ from the reference program's by a relative error of at most 0.0031.
Values may be sent and summed in bfloat16 or wider, within the bound.
No kernel may reach another device: no remote copies, remote signals or barrier semaphores. Data moves between devices by JAX's collectives and lax.ppermute only.
A program may use at most 128 MiB of HBM per device.

```python
import jax
import jax.numpy as jnp

D = 2048
FF = 4096
KERNEL = 3
TOK_DEV = 768
TOKENS = 12288


def raised(entries, key, source, target, blocks, factor):
    owner, partner = [(jnp.arange(entries.shape[axis_at]) // (entries.shape[axis_at] // blocks)).reshape([-1 if axis == axis_at else 1 for axis in range(entries.ndim)]) for axis_at in (source, target)]
    chosen = jax.random.permutation(key, blocks)[partner]
    strong = (owner == chosen) | (owner == (partner + blocks // 2) % blocks)
    return jnp.where(strong, factor * entries, entries)


def levels(rng, dims, cuts, low, high):
    gain, own = 1.0, jax.random.fold_in(rng, 6)
    for position, blocks in cuts:
        draws = jnp.exp(jax.random.uniform(jax.random.fold_in(own, position), (blocks,), jnp.float32, low / len(cuts), high / len(cuts)))
        gain = gain * jnp.repeat(draws, dims[position] // blocks).reshape([-1 if axis == position else 1 for axis in range(len(dims))])
    return gain


def bell_draw(own_key, shape, scale, limit, shards=(), kind=jnp.bfloat16):
    entries = scale * jax.random.normal(own_key, shape, jnp.float32)
    if shards:
        entries = entries * levels(own_key, shape, shards, -0.22, 0.18)
    return jnp.clip(entries, -limit, limit).astype(kind)


def heavy_noise(key, dims, deviation, most, pieces, heavy, kind=jnp.bfloat16):
    entries = deviation * jax.random.normal(key, dims, jnp.float32)
    if pieces:
        entries = entries * levels(key, dims, pieces, -0.22, 0.18)
    return jnp.clip(raised(entries, jax.random.fold_in(key, 3), *heavy), -most, most).astype(kind)


def setup_inputs(seed: int = 0) -> dict:
    seeds = jax.random.split(jax.random.key(seed), 9)
    return {
        "pre_gate": bell_draw(seeds[0], (TOKENS, FF), 1.0, 6.0, ((0, 16), (1, 2))),
        "pre_linear": bell_draw(seeds[1], (TOKENS, FF), 1.0, 6.0, ((0, 16), (1, 2))),
        "taps_gate": bell_draw(seeds[2], (KERNEL, FF), KERNEL ** -0.5, 3.5, ((1, 2),), jnp.float32),
        "taps_linear": bell_draw(seeds[3], (KERNEL, FF), KERNEL ** -0.5, 3.5, ((1, 2),), jnp.float32),
        "bias_gate": bell_draw(seeds[4], (FF,), 0.5, 3.0, ((0, 2),), jnp.float32),
        "bias_linear": bell_draw(seeds[5], (FF,), 0.5, 3.0, ((0, 2),), jnp.float32),
        "down_weight": bell_draw(seeds[6], (FF, D), FF ** -0.5, 0.09375, ((0, 2), (1, 8))),
        "out_grad": heavy_noise(seeds[7], (TOKENS, D), 1.0, 8.0, ((0, 16),), (0, 1, 16, 2.0)),
    }


def convolve(values, taps, bias):
    length = values.shape[1]
    padded = jnp.pad(values, ((0, 0), (2, 0), (0, 0)))
    return taps[0] * padded[:, 0:length] + taps[1] * padded[:, 1:length + 1] + taps[2] * padded[:, 2:length + 2] + bias


def convolve_back(grads, taps):
    length = grads.shape[1]
    padded = jnp.pad(grads, ((0, 0), (0, 2), (0, 0)))
    return taps[0] * padded[:, 2:length + 2] + taps[1] * padded[:, 1:length + 1] + taps[2] * padded[:, 0:length]


def tap_grads(grads, values):
    length = values.shape[1]
    padded = jnp.pad(values, ((0, 0), (2, 0), (0, 0)))
    return jnp.stack([jnp.sum(grads * padded[:, j:j + length], axis=(0, 1)) for j in range(3)])


def reference(pre_gate, pre_linear, taps_gate, taps_linear, bias_gate, bias_linear, down_weight, out_grad):
    seqs = pre_gate.shape[0] // TOK_DEV
    width = pre_gate.shape[1]
    gate_in = pre_gate.astype(jnp.float32).reshape(seqs, TOK_DEV, width)
    linear_in = pre_linear.astype(jnp.float32).reshape(seqs, TOK_DEV, width)
    gate_pre = convolve(gate_in, taps_gate, bias_gate)
    linear_pre = convolve(linear_in, taps_linear, bias_linear)
    sigma = jax.nn.sigmoid(gate_pre)
    silu_val = gate_pre * sigma
    hidden = (silu_val * linear_pre).astype(jnp.bfloat16).reshape(seqs * TOK_DEV, width)
    grad_hidden = jnp.dot(out_grad, down_weight.T, preferred_element_type=jnp.float32).reshape(seqs, TOK_DEV, width)
    grad_gate_pre = grad_hidden * linear_pre * sigma * (1.0 + gate_pre * (1.0 - sigma))
    grad_linear_pre = grad_hidden * silu_val
    grad_gate = convolve_back(grad_gate_pre, taps_gate).reshape(seqs * TOK_DEV, width).astype(jnp.bfloat16)
    grad_linear = convolve_back(grad_linear_pre, taps_linear).reshape(seqs * TOK_DEV, width).astype(jnp.bfloat16)
    grad_taps_gate = tap_grads(grad_gate_pre, gate_in)
    grad_taps_linear = tap_grads(grad_linear_pre, linear_in)
    grad_bias_gate = jnp.sum(grad_gate_pre, axis=(0, 1))
    grad_bias_linear = jnp.sum(grad_linear_pre, axis=(0, 1))
    grad_down = jnp.dot(hidden.T, out_grad, preferred_element_type=jnp.float32)
    row_norms = jnp.sum(grad_down * grad_down, axis=1)
    return (grad_gate, grad_linear, grad_taps_gate, grad_taps_linear, grad_bias_gate, grad_bias_linear, grad_down, row_norms)
```

```python
import functools

import jax
import jax.numpy as jnp
from jax import lax
from jax.experimental import pallas as pl
from jax.experimental.pallas import tpu as pltpu
from jax.sharding import PartitionSpec as P


HALVES = 2
GATE_CALLS = 2
F32, BF16 = jnp.float32, jnp.bfloat16


RING = 4


def swap(value, axis, size, distance):
    return lax.ppermute(value, axis, [(i, i ^ distance) for i in range(size)])


def ring(value, size, steps):
    inner = size // RING
    pairs = [(i, (i // inner + steps) % RING * inner + i % inner) for i in range(size)]
    return lax.ppermute(value, "fs", pairs)


def bits_below(size):
    return [1 << k for k in range(size.bit_length() - 1)]


def pair_sum(value, axis, size, distances):
    got = [swap(value, axis, size, d) for d in distances]
    if len(distances) == 1:
        return value + got[0]
    third = swap(value, axis, size, distances[0] ^ distances[1])
    return (value + got[0]) + (got[1] + third)


def lane_block(length):
    return min(length, 256)


def row_step(length):
    return 64 if length % 64 == 0 else 32 if length % 32 == 0 else 16


def hidden_kernel(block_rows, at_ref, gate_ref, linear_ref, tg_ref, tl_ref, bg_ref, bl_ref, out_ref, made):
    rows, lanes = gate_ref.shape
    step = row_step(block_rows)
    flip = at_ref[1]

    def convolved(ref, taps_ref, bias_ref, start, cols):
        now = ref[pl.ds(start, step), cols].astype(F32)
        back = pl.multiple_of(jnp.maximum(start - 16, 0), 16)
        halo = ref[pl.ds(back, 16), cols].astype(F32)[8:16]
        halo = jnp.where(start > 0, halo, 0.0)
        ext = jnp.concatenate([halo, now], 0)
        one, two = pltpu.roll(ext, 1, 0)[8:], pltpu.roll(ext, 2, 0)[8:]
        return (
            taps_ref[0:1, cols] * two
            + taps_ref[1:2, cols] * one
            + taps_ref[2:3, cols] * now
            + bias_ref[0:1, cols]
        )

    for lane in range(0, lanes, 128):
        cols = slice(lane, lane + 128)

        def body(i, carry):
            start = pl.multiple_of(i * step, step)
            g = convolved(gate_ref, tg_ref, bg_ref, start, cols)
            l = convolved(linear_ref, tl_ref, bl_ref, start, cols)
            block, rest = start // block_rows, start % block_rows
            to = pl.multiple_of((block ^ flip) * block_rows + rest, 16)
            made[pl.ds(to, step), cols] = (g * jax.nn.sigmoid(g) * l).astype(BF16)
            return carry

        lax.fori_loop(0, rows // step, body, 0, unroll=2)
    out_ref[...] = made[...].T


def hidden_half(which, flip, block_rows, pre_gate, pre_linear, taps_gate, taps_linear, bias_gate, bias_linear):
    rows, width = pre_gate.shape
    half = width // 2
    lanes = lane_block(half)
    steps = half // lanes
    wide = pl.BlockSpec((rows, lanes), lambda i, at: (0, at[0] * steps + i))
    taps = pl.BlockSpec((3, lanes), lambda i, at: (0, at[0] * steps + i))
    bias = pl.BlockSpec((1, lanes), lambda i, at: (0, at[0] * steps + i))
    return pl.pallas_call(
        functools.partial(hidden_kernel, block_rows),
        grid_spec=pltpu.PrefetchScalarGridSpec(
            num_scalar_prefetch=1,
            grid=(steps,),
            in_specs=[wide, wide, taps, taps, bias, bias],
            out_specs=pl.BlockSpec((lanes, rows), lambda i, at: (i, 0)),
            scratch_shapes=[pltpu.VMEM((rows, lanes), BF16)],
        ),
        out_shape=jax.ShapeDtypeStruct((half, rows), BF16),
        cost_estimate=pl.CostEstimate(
            flops=3000 * rows * half, bytes_accessed=6 * rows * half, transcendentals=rows * half
        ),
        name="hidden",
        compiler_params=pltpu.CompilerParams(vmem_limit_bytes=12 << 20),
    )(
        jnp.stack([which, flip]).astype(jnp.int32),
        pre_gate,
        pre_linear,
        taps_gate,
        taps_linear,
        bias_gate[None],
        bias_linear[None],
    )


def column_block(tokens, cols, index):
    if tokens.ndim == 3:
        return pl.BlockSpec((None, *tokens.shape[1:]), lambda j, at: (index(j, at), 0, 0))
    return pl.BlockSpec((tokens.shape[0], cols), lambda j, at: (0, index(j, at)))


def own_kernel(at_ref, hidden_ref, tokens_ref, out_ref):
    out_ref[...] = lax.dot_general(
        hidden_ref[...], tokens_ref[...], (((1,), (0,)), ((), ())), preferred_element_type=F32
    )


def own_blocks(blocks, cols, hidden, tokens):
    half, rows = hidden.shape
    count = len(blocks)
    return pl.pallas_call(
        own_kernel,
        grid_spec=pltpu.PrefetchScalarGridSpec(
            num_scalar_prefetch=1,
            grid=(count,),
            in_specs=[
                pl.BlockSpec((half, rows), lambda j, at: (0, 0)),
                column_block(tokens, cols, lambda j, at: at[j]),
            ],
            out_specs=pl.BlockSpec((None, half, cols), lambda j, at: (j, 0, 0)),
        ),
        out_shape=jax.ShapeDtypeStruct((count, half, cols), F32),
        compiler_params=pltpu.CompilerParams(vmem_limit_bytes=24 << 20),
        cost_estimate=pl.CostEstimate(
            flops=2 * rows * half * cols * count, bytes_accessed=2 * rows * (half + cols * count), transcendentals=0
        ),
        name="own",
    )(jnp.stack(blocks).astype(jnp.int32), hidden, tokens)


def outer_kernel(groups, kind, n_tokens, at_ref, hidden_ref, before_ref, *refs):
    tokens, outs = refs[:n_tokens], refs[n_tokens:]
    right = jnp.concatenate([t[...] for t in tokens], 0)
    made = before_ref[...] + lax.dot_general(
        hidden_ref[...], right, (((1,), (0,)), ((), ())), preferred_element_type=F32
    )
    made = made.astype(kind)
    rows = made.shape[0] // HALVES
    at = 0
    for h, counts in enumerate(groups):
        step = 0
        for count in counts:
            for slot in range(count):

                @pl.when(pl.program_id(0) == step)
                def _(at=at, slot=slot, h=h):
                    outs[at][slot] = made[h * rows : (h + 1) * rows]

                step += 1
            at += 1


def outer_blocks(groups, kind, blocks, cols, hidden, shares, before, first):
    half, rows = hidden.shape
    count = len(blocks)
    shapes = [(c, half // HALVES, cols) for counts in groups for c in counts]
    outs = pl.pallas_call(
        functools.partial(outer_kernel, groups, kind, len(shares)),
        grid_spec=pltpu.PrefetchScalarGridSpec(
            num_scalar_prefetch=1,
            grid=(count,),
            in_specs=[
                pl.BlockSpec((half, rows), lambda j, at: (0, 0)),
                pl.BlockSpec((None, half, cols), lambda j, at: (first + j, 0, 0)),
                *[column_block(t, cols, lambda j, at: at[j]) for t in shares],
            ],
            out_specs=[pl.BlockSpec(s, lambda j, at: (0, 0, 0)) for s in shapes],
        ),
        out_shape=[jax.ShapeDtypeStruct(s, kind) for s in shapes],
        compiler_params=pltpu.CompilerParams(vmem_limit_bytes=24 << 20),
        cost_estimate=pl.CostEstimate(
            flops=2 * rows * half * cols * count, bytes_accessed=2 * rows * (half + cols * count), transcendentals=0
        ),
        name="outer",
    )(jnp.stack(blocks).astype(jnp.int32), hidden, before, *shares)
    result, at = [], 0
    for counts in groups:
        result.append(outs[at : at + len(counts)])
        at += len(counts)
    return result


def gate_kernel(size, aliased, at_ref, tokens_ref, *refs):
    weights = refs[:size]
    gate_ref, linear_ref, tg_ref, tl_ref, bg_ref, bl_ref = refs[size : size + 6]
    gate_out, linear_out, sums_out, grads = refs[size + 6 + 3 * aliased :]
    rows, lanes = gate_ref.shape
    step = row_step(rows)
    cols = weights[0].shape[1]

    def block(p):
        at = at_ref[p]
        if len(tokens_ref.shape) == 3:
            return tokens_ref[at]
        return tokens_ref[:, pl.ds(pl.multiple_of(at * cols, cols), cols)]

    grads[...] = lax.dot_general(
        jnp.concatenate([block(p) for p in range(size)], 1),
        jnp.concatenate([w[...] for w in weights], 1),
        (((1,), (1,)), ((), ())),
        preferred_element_type=F32,
    )
    count = rows // step

    def fold(x):
        return jnp.sum(x.reshape(step // 8, 8, 128), axis=0)

    for lane in range(0, lanes, 128):
        here = slice(lane, lane + 128)

        def taps_at(ref, start):
            now = ref[pl.ds(start, step), here].astype(F32)
            back = pl.multiple_of(jnp.maximum(start - 16, 0), 16)
            halo = ref[pl.ds(back, 16), here].astype(F32)[8:16]
            halo = jnp.where(start > 0, halo, 0.0)
            ext = jnp.concatenate([halo, now], 0)
            return pltpu.roll(ext, 2, 0)[8:], pltpu.roll(ext, 1, 0)[8:], now

        def back(new, later, taps_ref):
            ext = jnp.concatenate([new, later], 0)
            one = pltpu.roll(ext, step + 7, 0)[:step]
            two = pltpu.roll(ext, step + 6, 0)[:step]
            return taps_ref[0:1, here] * two + taps_ref[1:2, here] * one + taps_ref[2:3, here] * new

        def body(i, carry):
            later_g, later_l, sums = carry
            start = pl.multiple_of((count - 1 - i) * step, step)
            g2, g1, g0 = taps_at(gate_ref, start)
            l2, l1, l0 = taps_at(linear_ref, start)
            gate_pre = tg_ref[0:1, here] * g2 + tg_ref[1:2, here] * g1 + tg_ref[2:3, here] * g0 + bg_ref[0:1, here]
            linear_pre = tl_ref[0:1, here] * l2 + tl_ref[1:2, here] * l1 + tl_ref[2:3, here] * l0 + bl_ref[0:1, here]
            sigma = jax.nn.sigmoid(gate_pre)
            grad = grads[pl.ds(start, step), here]
            d_gate = grad * linear_pre * sigma * (1.0 + gate_pre * (1.0 - sigma))
            d_linear = grad * (gate_pre * sigma)
            gate_out[pl.ds(start, step), here] = back(d_gate, later_g, tg_ref).astype(BF16)
            linear_out[pl.ds(start, step), here] = back(d_linear, later_l, tl_ref).astype(BF16)
            terms = (d_gate * g2, d_gate * g1, d_gate * g0, d_linear * l2, d_linear * l1, d_linear * l0, d_gate, d_linear)
            return d_gate[:8], d_linear[:8], tuple(s + fold(t) for s, t in zip(sums, terms))

        zero = jnp.zeros((8, 128), F32)
        _, _, sums = lax.fori_loop(0, count, body, (zero, zero, (zero,) * 8))
        sums_out[:, here] = jnp.concatenate([jnp.sum(s, axis=0, keepdims=True) for s in sums], 0)


def gate_part(call, tokens, index, own, others, pre_gate, pre_linear, taps_gate, taps_linear, bias_gate, bias_linear, before):
    rows, width = pre_gate.shape
    parts = HALVES * GATE_CALLS
    count = width // parts
    lanes = lane_block(count)
    steps = count // lanes
    cols = own.shape[1]
    inner = call % GATE_CALLS
    at = lambda i, s: (0, call * steps + i)
    wide = pl.BlockSpec((rows, lanes), at)
    aliased = before is not None
    extra = list(before) if aliased else []
    size = 1 + len(others)
    if tokens.ndim == 3:
        whole = pl.BlockSpec(tokens.shape, lambda i, s: (0, 0, 0))
    else:
        whole = pl.BlockSpec(tokens.shape, lambda i, s: (0, 0))
    return pl.pallas_call(
        functools.partial(gate_kernel, size, aliased),
        grid_spec=pltpu.PrefetchScalarGridSpec(
            num_scalar_prefetch=1,
            grid=(steps,),
            in_specs=[
                whole,
                pl.BlockSpec((lanes, cols), lambda i, s: (call * steps + i, 0)),
                *[pl.BlockSpec((lanes, cols), lambda i, s: (inner * steps + i, 0)) for _ in others],
                wide,
                wide,
                pl.BlockSpec((3, lanes), at),
                pl.BlockSpec((3, lanes), at),
                pl.BlockSpec((1, lanes), at),
                pl.BlockSpec((1, lanes), at),
                *[pl.BlockSpec(memory_space=pl.ANY) for _ in extra],
            ],
            out_specs=[wide, wide, pl.BlockSpec((8, lanes), at)],
            scratch_shapes=[pltpu.VMEM((rows, lanes), F32)],
        ),
        out_shape=[
            jax.ShapeDtypeStruct(pre_gate.shape, BF16),
            jax.ShapeDtypeStruct(pre_gate.shape, BF16),
            jax.ShapeDtypeStruct((8, width), F32),
        ],
        input_output_aliases={8 + size + j: j for j in range(len(extra))},
        cost_estimate=pl.CostEstimate(
            flops=5000 * rows * count, bytes_accessed=8 * rows * count, transcendentals=rows * count
        ),
        name="gate",
        compiler_params=pltpu.CompilerParams(vmem_limit_bytes=20 << 20),
    )(
        index,
        tokens,
        own,
        *others,
        pre_gate,
        pre_linear,
        taps_gate,
        taps_linear,
        bias_gate[None],
        bias_linear[None],
        *extra,
    )


def local(sizes, pre_gate, pre_linear, taps_gate, taps_linear, bias_gate, bias_linear, down_weight, out_grad):
    fs, tp = sizes["fs"], sizes["tp"]
    inner = fs // RING
    rep_at, fs_at, tp_at = (lax.axis_index(a) for a in ("rep", "fs", "tp"))
    out_at, in_at = fs_at // inner, fs_at % inner
    cols = out_grad.shape[1] // fs
    params = (pre_gate, pre_linear, taps_gate, taps_linear, bias_gate, bias_linear)

    def block_at(d, q):
        return (out_at + d) % RING * inner + (in_at ^ q)

    def blocked(tokens):
        if cols % 128 == 0:
            return tokens
        return tokens.reshape(tokens.shape[0], fs, cols).transpose(1, 0, 2)

    rows = out_grad.shape[0] // tp
    share = swap(lax.dynamic_slice_in_dim(out_grad, tp_at * rows, rows, 0), "rep", 2, 1)

    to_send = hidden_half(1 - rep_at, tp_at, rows, *params)
    arrived = swap(to_send, "rep", 2, 1)
    kept = hidden_half(rep_at, jnp.zeros_like(tp_at), rows, *params)

    w_rows = down_weight.shape[0] // HALVES
    late, _ = lax.optimization_barrier((down_weight, to_send))
    halves = [down_weight[:w_rows], late[w_rows:]]
    pieces = []
    for h in range(HALVES):
        have = {(0, 0): halves[h]}
        have[1, 0] = ring(have[0, 0], fs, 1)
        have[3, 0] = ring(have[0, 0], fs, -1)
        have[2, 0] = ring(have[1, 0], fs, 1)
        for q in range(1, inner):
            for d in (0, 1, 3, 2):
                if h and d == 2 and q == inner - 1:
                    have[d, q] = ring(have[1, q], fs, 1)
                else:
                    rest = q & (q - 1)
                    have[d, q] = swap(have[d, rest], "fs", fs, q ^ rest)
        pieces.append(have)

    shares = [share]
    for distance in bits_below(tp):
        shares = shares + [swap(v, "tp", tp, distance) for v in shares]
    shares = [blocked(t) for t in shares]
    tokens = blocked(out_grad)

    even = range(0, inner, 2)
    kept_places = [(d, q) for d in (2, 3, 1, 0) for q in even]
    held_blocks = [block_at(d, q) for d, q in kept_places]
    sent_blocks = [block_at(d, q ^ 1) for d, q in kept_places]
    count = len(even)
    groups = [[2 * count, 2 * count], [2 * count, count, count]]
    mine = own_blocks(sent_blocks + held_blocks, cols, kept, tokens)
    sent = outer_blocks(groups, BF16, sent_blocks, cols, arrived, shares, mine, 0)
    held = outer_blocks(groups, F32, held_blocks, cols, arrived, shares, mine, len(sent_blocks))
    finished = []
    for h in range(HALVES):
        sums = {}
        start = 0
        for keep, send in zip(held[h], sent[h]):
            both = keep + swap(send, "fs", fs, 1).astype(F32)
            sums.update({place: both[j] for j, place in enumerate(kept_places[start : start + both.shape[0]])})
            start += both.shape[0]
        for bit in bits_below(inner)[1:]:
            for d in range(RING):
                for q in even:
                    if q & -q == bit:
                        got = swap(sums[d, q].astype(BF16), "fs", fs, bit)
                        sums[d, q ^ bit] = sums[d, q ^ bit] + got.astype(F32)
        two = ring(sums[2, 0].astype(BF16), fs, 1)
        three = ring(sums[3, 0].astype(BF16), fs, -1)
        one = ring((sums[1, 0] + two.astype(F32)).astype(BF16), fs, 1)
        finished.append(sums[0, 0] + three.astype(F32) + one.astype(F32))
    theirs = [swap(v, "rep", 2, 1) for v in finished]
    first = rep_at == 0
    grad_down = jnp.concatenate(
        [jnp.where(first, v, w) for v, w in zip(finished, theirs)]
        + [jnp.where(first, w, v) for v, w in zip(finished, theirs)],
        0,
    )

    outs = None
    places = [(d, q) for q in range(inner) for d in (0, 1, 3, 2)]
    index = jnp.stack([block_at(-d, q) for d, q in places]).astype(jnp.int32)
    for call in range(HALVES * GATE_CALLS):
        others = [pieces[call // GATE_CALLS][place] for place in places[1:]]
        outs = gate_part(call, tokens, index, down_weight, others, *params, outs)
    grad_gate, grad_linear, packed = outs

    squares = jnp.concatenate([jnp.sum(v * v, axis=1) for v in finished])
    width = packed.shape[1]
    value = jnp.concatenate([packed, squares.reshape(8, -1)], 1)
    everyone = ("rep", "fs")
    spans = bits_below(fs)[::-1]
    pairs = len(spans) // 2
    for j in range(pairs):
        value = pair_sum(value, everyone, 2 * fs, spans[2 * j : 2 * j + 2])
    there = swap(value, everyone, 2 * fs, fs)
    for span in spans[2 * pairs :]:
        there = there + swap(value, everyone, 2 * fs, fs ^ span)
        value = value + swap(value, everyone, 2 * fs, span)
    packed = value[:, :width] + there[:, :width]
    norm, norm2 = value[:, width:].reshape(-1), there[:, width:].reshape(-1)
    row_norms = jnp.concatenate([jnp.where(first, norm, norm2), jnp.where(first, norm2, norm)], 0)
    return grad_gate, grad_linear, packed[0:3], packed[3:6], packed[6], packed[7], grad_down, row_norms


def solution(mesh):
    sizes = dict(mesh.shape)
    in_specs = (
        P(("rep", "fs"), "tp"),
        P(("rep", "fs"), "tp"),
        P(None, "tp"),
        P(None, "tp"),
        P("tp"),
        P("tp"),
        P("tp", "fs"),
        P(("rep", "fs"), None),
    )
    out_specs = (
        P(("rep", "fs"), "tp"),
        P(("rep", "fs"), "tp"),
        P(None, "tp"),
        P(None, "tp"),
        P("tp"),
        P("tp"),
        P("tp", "fs"),
        P("tp"),
    )

    def body(*args):
        return local(sizes, *args)

    return jax.shard_map(body, mesh=mesh, in_specs=in_specs, out_specs=out_specs, check_vma=False)
```

```python
import functools

import jax
import jax.numpy as jnp
from jax import lax
from jax.experimental import pallas as pl
from jax.experimental.pallas import tpu as pltpu
from jax.sharding import PartitionSpec as P


HALVES = 2
GATE_CALLS = 2
F32, BF16 = jnp.float32, jnp.bfloat16


RING = 4


def swap(value, axis, size, distance):
    return lax.ppermute(value, axis, [(i, i ^ distance) for i in range(size)])


def ring(value, size, steps):
    inner = size // RING
    pairs = [(i, (i // inner + steps) % RING * inner + i % inner) for i in range(size)]
    return lax.ppermute(value, "fs", pairs)


def bits_below(size):
    return [1 << k for k in range(size.bit_length() - 1)]


def pair_sum(value, axis, size, distances):
    got = [swap(value, axis, size, d) for d in distances]
    if len(distances) == 1:
        return value + got[0]
    third = swap(value, axis, size, distances[0] ^ distances[1])
    return (value + got[0]) + (got[1] + third)


def lane_block(length):
    return min(length, 256)


def row_step(length):
    return 64 if length % 64 == 0 else 32 if length % 32 == 0 else 16


def hidden_kernel(block_rows, at_ref, gate_ref, linear_ref, tg_ref, tl_ref, bg_ref, bl_ref, out_ref, made):
    rows, lanes = gate_ref.shape
    step = row_step(block_rows)
    flip = at_ref[1]

    def convolved(ref, taps_ref, bias_ref, start, cols):
        now = ref[pl.ds(start, step), cols].astype(F32)
        back = pl.multiple_of(jnp.maximum(start - 16, 0), 16)
        halo = ref[pl.ds(back, 16), cols].astype(F32)[8:16]
        halo = jnp.where(start > 0, halo, 0.0)
        ext = jnp.concatenate([halo, now], 0)
        one, two = pltpu.roll(ext, 1, 0)[8:], pltpu.roll(ext, 2, 0)[8:]
        return (
            taps_ref[0:1, cols] * two
            + taps_ref[1:2, cols] * one
            + taps_ref[2:3, cols] * now
            + bias_ref[0:1, cols]
        )

    for lane in range(0, lanes, 128):
        cols = slice(lane, lane + 128)

        def body(i, carry):
            start = pl.multiple_of(i * step, step)
            g = convolved(gate_ref, tg_ref, bg_ref, start, cols)
            l = convolved(linear_ref, tl_ref, bl_ref, start, cols)
            block, rest = start // block_rows, start % block_rows
            to = pl.multiple_of((block ^ flip) * block_rows + rest, 16)
            made[pl.ds(to, step), cols] = (g * jax.nn.sigmoid(g) * l).astype(BF16)
            return carry

        lax.fori_loop(0, rows // step, body, 0, unroll=4)
    out_ref[...] = made[...].T


def hidden_half(which, flip, block_rows, pre_gate, pre_linear, taps_gate, taps_linear, bias_gate, bias_linear):
    rows, width = pre_gate.shape
    half = width // 2
    lanes = lane_block(half)
    steps = half // lanes
    wide = pl.BlockSpec((rows, lanes), lambda i, at: (0, at[0] * steps + i))
    taps = pl.BlockSpec((3, lanes), lambda i, at: (0, at[0] * steps + i))
    bias = pl.BlockSpec((1, lanes), lambda i, at: (0, at[0] * steps + i))
    return pl.pallas_call(
        functools.partial(hidden_kernel, block_rows),
        grid_spec=pltpu.PrefetchScalarGridSpec(
            num_scalar_prefetch=1,
            grid=(steps,),
            in_specs=[wide, wide, taps, taps, bias, bias],
            out_specs=pl.BlockSpec((lanes, rows), lambda i, at: (i, 0)),
            scratch_shapes=[pltpu.VMEM((rows, lanes), BF16)],
        ),
        out_shape=jax.ShapeDtypeStruct((half, rows), BF16),
        cost_estimate=pl.CostEstimate(
            flops=3000 * rows * half, bytes_accessed=6 * rows * half, transcendentals=rows * half
        ),
        name="hidden",
        compiler_params=pltpu.CompilerParams(vmem_limit_bytes=12 << 20),
    )(
        jnp.stack([which, flip]).astype(jnp.int32),
        pre_gate,
        pre_linear,
        taps_gate,
        taps_linear,
        bias_gate[None],
        bias_linear[None],
    )


def column_block(tokens, cols, index):
    if tokens.ndim == 3:
        return pl.BlockSpec((None, *tokens.shape[1:]), lambda j, at: (index(j, at), 0, 0))
    return pl.BlockSpec((tokens.shape[0], cols), lambda j, at: (0, index(j, at)))


def own_kernel(at_ref, hidden_ref, tokens_ref, out_ref):
    out_ref[...] = lax.dot_general(
        hidden_ref[...], tokens_ref[...], (((1,), (0,)), ((), ())), preferred_element_type=F32
    )


def own_blocks(blocks, cols, hidden, tokens):
    half, rows = hidden.shape
    count = len(blocks)
    return pl.pallas_call(
        own_kernel,
        grid_spec=pltpu.PrefetchScalarGridSpec(
            num_scalar_prefetch=1,
            grid=(count,),
            in_specs=[
                pl.BlockSpec((half, rows), lambda j, at: (0, 0)),
                column_block(tokens, cols, lambda j, at: at[j]),
            ],
            out_specs=pl.BlockSpec((None, half, cols), lambda j, at: (j, 0, 0)),
        ),
        out_shape=jax.ShapeDtypeStruct((count, half, cols), F32),
        compiler_params=pltpu.CompilerParams(vmem_limit_bytes=24 << 20),
        cost_estimate=pl.CostEstimate(
            flops=2 * rows * half * cols * count, bytes_accessed=2 * rows * (half + cols * count), transcendentals=0
        ),
        name="own",
    )(jnp.stack(blocks).astype(jnp.int32), hidden, tokens)


def outer_kernel(groups, kind, n_tokens, at_ref, hidden_ref, before_ref, *refs):
    tokens, outs = refs[:n_tokens], refs[n_tokens:]
    right = jnp.concatenate([t[...] for t in tokens], 0)
    made = before_ref[...] + lax.dot_general(
        hidden_ref[...], right, (((1,), (0,)), ((), ())), preferred_element_type=F32
    )
    made = made.astype(kind)
    rows = made.shape[0] // HALVES
    at = 0
    for h, counts in enumerate(groups):
        step = 0
        for count in counts:
            for slot in range(count):

                @pl.when(pl.program_id(0) == step)
                def _(at=at, slot=slot, h=h):
                    outs[at][slot] = made[h * rows : (h + 1) * rows]

                step += 1
            at += 1


def outer_blocks(groups, kind, blocks, cols, hidden, shares, before, first):
    half, rows = hidden.shape
    count = len(blocks)
    shapes = [(c, half // HALVES, cols) for counts in groups for c in counts]
    outs = pl.pallas_call(
        functools.partial(outer_kernel, groups, kind, len(shares)),
        grid_spec=pltpu.PrefetchScalarGridSpec(
            num_scalar_prefetch=1,
            grid=(count,),
            in_specs=[
                pl.BlockSpec((half, rows), lambda j, at: (0, 0)),
                pl.BlockSpec((None, half, cols), lambda j, at: (first + j, 0, 0)),
                *[column_block(t, cols, lambda j, at: at[j]) for t in shares],
            ],
            out_specs=[pl.BlockSpec(s, lambda j, at: (0, 0, 0)) for s in shapes],
        ),
        out_shape=[jax.ShapeDtypeStruct(s, kind) for s in shapes],
        compiler_params=pltpu.CompilerParams(vmem_limit_bytes=24 << 20),
        cost_estimate=pl.CostEstimate(
            flops=2 * rows * half * cols * count, bytes_accessed=2 * rows * (half + cols * count), transcendentals=0
        ),
        name="outer",
    )(jnp.stack(blocks).astype(jnp.int32), hidden, before, *shares)
    result, at = [], 0
    for counts in groups:
        result.append(outs[at : at + len(counts)])
        at += len(counts)
    return result


def gate_kernel(size, aliased, at_ref, tokens_ref, *refs):
    weights = refs[:size]
    gate_ref, linear_ref, tg_ref, tl_ref, bg_ref, bl_ref = refs[size : size + 6]
    gate_out, linear_out, sums_out, grads = refs[size + 6 + 3 * aliased :]
    rows, lanes = gate_ref.shape
    step = row_step(rows)
    cols = weights[0].shape[1]

    def block(p):
        at = at_ref[p]
        if len(tokens_ref.shape) == 3:
            return tokens_ref[at]
        return tokens_ref[:, pl.ds(pl.multiple_of(at * cols, cols), cols)]

    grads[...] = lax.dot_general(
        jnp.concatenate([block(p) for p in range(size)], 1),
        jnp.concatenate([w[...] for w in weights], 1),
        (((1,), (1,)), ((), ())),
        preferred_element_type=F32,
    )
    count = rows // step

    def fold(x):
        return jnp.sum(x.reshape(step // 8, 8, 128), axis=0)

    for lane in range(0, lanes, 128):
        here = slice(lane, lane + 128)

        def taps_at(ref, start):
            now = ref[pl.ds(start, step), here].astype(F32)
            back = pl.multiple_of(jnp.maximum(start - 16, 0), 16)
            halo = ref[pl.ds(back, 16), here].astype(F32)[8:16]
            halo = jnp.where(start > 0, halo, 0.0)
            ext = jnp.concatenate([halo, now], 0)
            return pltpu.roll(ext, 2, 0)[8:], pltpu.roll(ext, 1, 0)[8:], now

        def back(new, later, taps_ref):
            ext = jnp.concatenate([new, later], 0)
            one = pltpu.roll(ext, step + 7, 0)[:step]
            two = pltpu.roll(ext, step + 6, 0)[:step]
            return taps_ref[0:1, here] * two + taps_ref[1:2, here] * one + taps_ref[2:3, here] * new

        def body(i, carry):
            later_g, later_l, sums = carry
            start = pl.multiple_of((count - 1 - i) * step, step)
            g2, g1, g0 = taps_at(gate_ref, start)
            l2, l1, l0 = taps_at(linear_ref, start)
            gate_pre = tg_ref[0:1, here] * g2 + tg_ref[1:2, here] * g1 + tg_ref[2:3, here] * g0 + bg_ref[0:1, here]
            linear_pre = tl_ref[0:1, here] * l2 + tl_ref[1:2, here] * l1 + tl_ref[2:3, here] * l0 + bl_ref[0:1, here]
            sigma = jax.nn.sigmoid(gate_pre)
            grad = grads[pl.ds(start, step), here]
            silu = gate_pre * sigma
            d_gate = grad * linear_pre * (sigma + silu * (1.0 - sigma))
            d_linear = grad * silu
            gate_out[pl.ds(start, step), here] = back(d_gate, later_g, tg_ref).astype(BF16)
            linear_out[pl.ds(start, step), here] = back(d_linear, later_l, tl_ref).astype(BF16)
            terms = (d_gate * g2, d_gate * g1, d_gate * g0, d_linear * l2, d_linear * l1, d_linear * l0, d_gate, d_linear)
            return d_gate[:8], d_linear[:8], tuple(s + fold(t) for s, t in zip(sums, terms))

        zero = jnp.zeros((8, 128), F32)
        _, _, sums = lax.fori_loop(0, count, body, (zero, zero, (zero,) * 8))
        sums_out[:, here] = jnp.concatenate([jnp.sum(s, axis=0, keepdims=True) for s in sums], 0)


def gate_part(call, tokens, index, own, others, pre_gate, pre_linear, taps_gate, taps_linear, bias_gate, bias_linear, before):
    rows, width = pre_gate.shape
    parts = HALVES * GATE_CALLS
    count = width // parts
    lanes = lane_block(count)
    steps = count // lanes
    cols = own.shape[1]
    inner = call % GATE_CALLS
    at = lambda i, s: (0, call * steps + i)
    wide = pl.BlockSpec((rows, lanes), at)
    aliased = before is not None
    extra = list(before) if aliased else []
    size = 1 + len(others)
    if tokens.ndim == 3:
        whole = pl.BlockSpec(tokens.shape, lambda i, s: (0, 0, 0))
    else:
        whole = pl.BlockSpec(tokens.shape, lambda i, s: (0, 0))
    return pl.pallas_call(
        functools.partial(gate_kernel, size, aliased),
        grid_spec=pltpu.PrefetchScalarGridSpec(
            num_scalar_prefetch=1,
            grid=(steps,),
            in_specs=[
                whole,
                pl.BlockSpec((lanes, cols), lambda i, s: (call * steps + i, 0)),
                *[pl.BlockSpec((lanes, cols), lambda i, s: (inner * steps + i, 0)) for _ in others],
                wide,
                wide,
                pl.BlockSpec((3, lanes), at),
                pl.BlockSpec((3, lanes), at),
                pl.BlockSpec((1, lanes), at),
                pl.BlockSpec((1, lanes), at),
                *[pl.BlockSpec(memory_space=pl.ANY) for _ in extra],
            ],
            out_specs=[wide, wide, pl.BlockSpec((8, lanes), at)],
            scratch_shapes=[pltpu.VMEM((rows, lanes), F32)],
        ),
        out_shape=[
            jax.ShapeDtypeStruct(pre_gate.shape, BF16),
            jax.ShapeDtypeStruct(pre_gate.shape, BF16),
            jax.ShapeDtypeStruct((8, width), F32),
        ],
        input_output_aliases={8 + size + j: j for j in range(len(extra))},
        cost_estimate=pl.CostEstimate(
            flops=5000 * rows * count, bytes_accessed=8 * rows * count, transcendentals=rows * count
        ),
        name="gate",
        compiler_params=pltpu.CompilerParams(vmem_limit_bytes=20 << 20),
    )(
        index,
        tokens,
        own,
        *others,
        pre_gate,
        pre_linear,
        taps_gate,
        taps_linear,
        bias_gate[None],
        bias_linear[None],
        *extra,
    )


def local(sizes, pre_gate, pre_linear, taps_gate, taps_linear, bias_gate, bias_linear, down_weight, out_grad):
    fs, tp = sizes["fs"], sizes["tp"]
    inner = fs // RING
    rep_at, fs_at, tp_at = (lax.axis_index(a) for a in ("rep", "fs", "tp"))
    out_at, in_at = fs_at // inner, fs_at % inner
    cols = out_grad.shape[1] // fs
    params = (pre_gate, pre_linear, taps_gate, taps_linear, bias_gate, bias_linear)

    def block_at(d, q):
        return (out_at + d) % RING * inner + (in_at ^ q)

    def blocked(tokens):
        if cols % 128 == 0:
            return tokens
        return tokens.reshape(tokens.shape[0], fs, cols).transpose(1, 0, 2)

    rows = out_grad.shape[0] // tp
    share = swap(lax.dynamic_slice_in_dim(out_grad, tp_at * rows, rows, 0), "rep", 2, 1)

    to_send = hidden_half(1 - rep_at, tp_at, rows, *params)
    arrived = swap(to_send, "rep", 2, 1)
    kept = hidden_half(rep_at, jnp.zeros_like(tp_at), rows, *params)

    w_rows = down_weight.shape[0] // HALVES
    late, _ = lax.optimization_barrier((down_weight, to_send))
    halves = [down_weight[:w_rows], late[w_rows:]]
    pieces = []
    for h in range(HALVES):
        have = {(0, 0): halves[h]}
        have[1, 0] = ring(have[0, 0], fs, 1)
        have[3, 0] = ring(have[0, 0], fs, -1)
        have[2, 0] = ring(have[1, 0], fs, 1)
        for q in range(1, inner):
            for d in (0, 1, 3, 2):
                if h and d == 2 and q == inner - 1:
                    have[d, q] = ring(have[1, q], fs, 1)
                else:
                    rest = q & (q - 1)
                    have[d, q] = swap(have[d, rest], "fs", fs, q ^ rest)
        pieces.append(have)

    shares = [share]
    for distance in bits_below(tp):
        shares = shares + [swap(v, "tp", tp, distance) for v in shares]
    shares = [blocked(t) for t in shares]
    tokens = blocked(out_grad)

    even = range(0, inner, 2)
    kept_places = [(d, q) for d in (2, 3, 1, 0) for q in even]
    held_blocks = [block_at(d, q) for d, q in kept_places]
    sent_blocks = [block_at(d, q ^ 1) for d, q in kept_places]
    count = len(even)
    groups = [[2 * count, 2 * count], [2 * count, count, count]]
    mine = own_blocks(sent_blocks + held_blocks, cols, kept, tokens)
    sent = outer_blocks(groups, BF16, sent_blocks, cols, arrived, shares, mine, 0)
    held = outer_blocks(groups, F32, held_blocks, cols, arrived, shares, mine, len(sent_blocks))
    finished = []
    for h in range(HALVES):
        sums = {}
        start = 0
        for keep, send in zip(held[h], sent[h]):
            both = keep + swap(send, "fs", fs, 1).astype(F32)
            sums.update({place: both[j] for j, place in enumerate(kept_places[start : start + both.shape[0]])})
            start += both.shape[0]
        for bit in bits_below(inner)[1:]:
            for d in range(RING):
                for q in even:
                    if q & -q == bit:
                        got = swap(sums[d, q].astype(BF16), "fs", fs, bit)
                        sums[d, q ^ bit] = sums[d, q ^ bit] + got.astype(F32)
        two = ring(sums[2, 0].astype(BF16), fs, 1)
        three = ring(sums[3, 0].astype(BF16), fs, -1)
        one = ring((sums[1, 0] + two.astype(F32)).astype(BF16), fs, 1)
        finished.append(sums[0, 0] + three.astype(F32) + one.astype(F32))
    theirs = [swap(v, "rep", 2, 1) for v in finished]
    first = rep_at == 0
    grad_down = jnp.concatenate(
        [jnp.where(first, v, w) for v, w in zip(finished, theirs)]
        + [jnp.where(first, w, v) for v, w in zip(finished, theirs)],
        0,
    )

    outs = None
    places = [(d, q) for q in range(inner) for d in (0, 1, 3, 2)]
    index = jnp.stack([block_at(-d, q) for d, q in places]).astype(jnp.int32)
    for call in range(HALVES * GATE_CALLS):
        others = [pieces[call // GATE_CALLS][place] for place in places[1:]]
        outs = gate_part(call, tokens, index, down_weight, others, *params, outs)
    grad_gate, grad_linear, packed = outs

    squares = jnp.concatenate([jnp.sum(v * v, axis=1) for v in finished])
    width = packed.shape[1]
    value = jnp.concatenate([packed, squares.reshape(8, -1)], 1)
    everyone = ("rep", "fs")
    spans = bits_below(fs)[::-1]
    pairs = len(spans) // 2
    for j in range(pairs):
        value = pair_sum(value, everyone, 2 * fs, spans[2 * j : 2 * j + 2])
    there = swap(value, everyone, 2 * fs, fs)
    for span in spans[2 * pairs :]:
        there = there + swap(value, everyone, 2 * fs, fs ^ span)
        value = value + swap(value, everyone, 2 * fs, span)
    packed = value[:, :width] + there[:, :width]
    norm, norm2 = value[:, width:].reshape(-1), there[:, width:].reshape(-1)
    row_norms = jnp.concatenate([jnp.where(first, norm, norm2), jnp.where(first, norm2, norm)], 0)
    return grad_gate, grad_linear, packed[0:3], packed[3:6], packed[6], packed[7], grad_down, row_norms


def solution(mesh):
    sizes = dict(mesh.shape)
    in_specs = (
        P(("rep", "fs"), "tp"),
        P(("rep", "fs"), "tp"),
        P(None, "tp"),
        P(None, "tp"),
        P("tp"),
        P("tp"),
        P("tp", "fs"),
        P(("rep", "fs"), None),
    )
    out_specs = (
        P(("rep", "fs"), "tp"),
        P(("rep", "fs"), "tp"),
        P(None, "tp"),
        P(None, "tp"),
        P("tp"),
        P("tp"),
        P("tp", "fs"),
        P("tp"),
    )

    def body(*args):
        return local(sizes, *args)

    return jax.shard_map(body, mesh=mesh, in_specs=in_specs, out_specs=out_specs, check_vma=False)
```
